32 devices in a mesh: ra: 4 (over z), cb: 4 (over y, x), dp: 2 (over core).
Axes of the slice: x: 2, y: 2, z: 4, core: 2. Of those that a mesh axis runs over, the one named last changes fastest.
Arguments:
- stream: bfloat16 [4, 64, 4096], P('dp', None, 'ra'), may hold values from -16 to 16
- norm_gain: bfloat16 [2, 4096], P(None, 'ra'), may hold values from 0.099609375 to 1.8984375
- gate_weight: bfloat16 [2, 4096, 12288], P(None, 'ra', 'cb'), may hold values from -0.09375 to 0.09375
- value_weight: bfloat16 [2, 4096, 12288], P(None, 'ra', 'cb'), may hold values from -0.09375 to 0.09375
- gate_taps: bfloat16 [2, 3, 12288], P(None, None, 'cb'), may hold values from -3 to 3
- value_taps: bfloat16 [2, 3, 12288], P(None, None, 'cb'), may hold values from -3 to 3
- gate_bias: bfloat16 [2, 12288], P(None, 'cb'), may hold values from -3 to 3
- value_bias: bfloat16 [2, 12288], P(None, 'cb'), may hold values from -3 to 3
- down_weight: bfloat16 [2, 12288, 4096], P(None, 'cb', 'ra'), may hold values from -0.0546875 to 0.0546875
- final_gain: bfloat16 [4096], P('ra'), may hold values from 0.099609375 to 1.8984375
Outputs:
- mixed: bfloat16 [4, 64, 4096], P('dp', None, 'ra')
The draws below stay inside these ranges and needn't reach their ends.
All inputs are finite; a program needn't handle non-finite values.
Results may differ from the reference program's by a relative error of at most 0.035.
Values may be sent and summed in bfloat16 or wider, within the bound.
A program may use at most 128 MiB of HBM per device.

```python
import jax
import jax.numpy as jnp
from jax import lax

D = 4096
FF = 12288
TAPS = 3
LAYERS = 2
LEN = 64
BATCH = 4
N_CB = 4


def draw_stream(key, part):
    first, second, third = jax.random.split(key, 3)
    base = jnp.clip(jax.random.normal(first, (BATCH, LEN, D), jnp.float32), -4.0, 4.0)
    channel = jnp.exp(jax.random.uniform(second, (D // 16,), jnp.float32, -1.1, 1.1))
    rowscale = jnp.exp(jax.random.uniform(third, (BATCH, LEN), jnp.float32, -0.7, 0.7))
    values = base * jnp.repeat(channel, 16)[None, None, :] * rowscale[:, :, None]
    return jnp.clip(values, -16.0, 16.0).astype(jnp.bfloat16)


def steps_of(rng, extent, cuts, smallest, largest):
    def one(position, blocks):
        heights = jax.random.uniform(jax.random.fold_in(jax.random.fold_in(rng, 6), position), (blocks,), jnp.float32, smallest / len(cuts), largest / len(cuts))
        return jnp.repeat(jnp.exp(heights), extent[position] // blocks).reshape((-1,) + (1,) * (len(extent) - position - 1))

    gain = one(*cuts[0])
    for cut in cuts[1:]:
        gain = gain * one(*cut)
    return gain


def bell_draw(stream_key, shape, spread, most, shards=(), kind=jnp.bfloat16):
    values = spread * jax.random.normal(stream_key, shape, jnp.float32)
    if shards:
        values = values * steps_of(stream_key, shape, shards, -0.22, 0.18)
    return jnp.clip(values, -most, most).astype(kind)


def setup_inputs(seed: int = 0) -> dict:
    keys = jax.random.split(jax.random.key(seed), 11)
    stream = draw_stream(jax.random.fold_in(keys[10], 71), 0)
    norm_gain = jnp.clip(1.0 + 0.18 * jax.random.normal(keys[1], (LAYERS, D), jnp.float32), 0.099609375, 1.8984375).astype(jnp.bfloat16)
    gate_weight = bell_draw(keys[2], (LAYERS, D, FF), D ** -0.5, 0.09375, ((1, 4), (2, 4)))
    value_weight = bell_draw(keys[3], (LAYERS, D, FF), D ** -0.5, 0.09375, ((1, 4), (2, 4)))
    gate_taps = bell_draw(keys[4], (LAYERS, TAPS, FF), 0.577, 3.0, ((2, 4),))
    value_taps = bell_draw(keys[5], (LAYERS, TAPS, FF), 0.577, 3.0, ((2, 4),))
    gate_bias = bell_draw(keys[6], (LAYERS, FF), 0.5, 3.0, ((1, 4),))
    value_bias = bell_draw(keys[7], (LAYERS, FF), 0.5, 3.0, ((1, 4),))
    down_weight = bell_draw(keys[8], (LAYERS, FF, D), FF ** -0.5, 0.0546875, ((1, 4), (2, 4)))
    final_gain = jnp.clip(1.0 + 0.18 * jax.random.normal(keys[9], (D,), jnp.float32), 0.099609375, 1.8984375).astype(jnp.bfloat16)
    return dict(stream=stream, norm_gain=norm_gain, gate_weight=gate_weight, value_weight=value_weight, gate_taps=gate_taps, value_taps=value_taps, gate_bias=gate_bias, value_bias=value_bias, down_weight=down_weight, final_gain=final_gain)


EPS = 1e-06

def rms_scaled(stream_in, gain_row):
    values = stream_in.astype(jnp.float32)
    squares = lax.optimization_barrier(jnp.sum(values * values, axis=-1, keepdims=True))
    return values * lax.rsqrt(squares / D + EPS) * gain_row.astype(jnp.float32)

def causal_mix(up_rows, taps, bias):
    length = up_rows.shape[1]
    count = taps.shape[0]
    padded = jnp.pad(up_rows.astype(jnp.float32), ((0, 0), (count - 1, 0), (0, 0)))
    result = jnp.zeros(up_rows.shape, jnp.float32) + bias.astype(jnp.float32)
    for tap_index in range(count):
        result = result + padded[:, tap_index:tap_index + length] * taps[tap_index].astype(jnp.float32)
    return result

def reference(stream, norm_gain, gate_weight, value_weight, gate_taps, value_taps, gate_bias, value_bias, down_weight, final_gain):
    batch_rows, length, width = stream.shape
    current = stream
    ff_block = FF // N_CB
    for layer_index in range(LAYERS):
        normed = rms_scaled(current, norm_gain[layer_index]).astype(jnp.bfloat16).reshape(-1, width)
        gate_up = jnp.dot(normed, gate_weight[layer_index], preferred_element_type=jnp.float32).astype(jnp.bfloat16)
        value_up = jnp.dot(normed, value_weight[layer_index], preferred_element_type=jnp.float32).astype(jnp.bfloat16)
        gate_conv = causal_mix(gate_up.reshape(batch_rows, length, FF), gate_taps[layer_index], gate_bias[layer_index])
        value_conv = causal_mix(value_up.reshape(batch_rows, length, FF), value_taps[layer_index], value_bias[layer_index])
        hidden = (jax.nn.gelu(gate_conv) * value_conv).astype(jnp.bfloat16).reshape(-1, FF)
        branch = jnp.zeros((hidden.shape[0], width), jnp.float32)
        for block_index in range(N_CB):
            lower = block_index * ff_block
            term = jnp.dot(hidden[:, lower:lower + ff_block], down_weight[layer_index, lower:lower + ff_block], preferred_element_type=jnp.float32)
            rounded = lax.optimization_barrier(term.astype(jnp.bfloat16))
            branch = branch + rounded.astype(jnp.float32)
        current = (0.5 * current.astype(jnp.float32) + branch.reshape(batch_rows, length, width)).astype(jnp.bfloat16)
    return rms_scaled(current, final_gain).astype(jnp.bfloat16)
```

```python
import functools

import jax
import jax.numpy as jnp
from jax import lax
from jax.experimental import pallas as pl
from jax.experimental.pallas import tpu as pltpu
from jax.sharding import PartitionSpec as P

EPS = 1e-06
MESH = pl.DeviceIdType.MESH
LANES = 128
GROUPS = 2
CHUNKS = 6
SKEW = 2
SKEW_BACK = 2
SKEW_CB = 2


def chain_kernel(
    dims,
    s_in, ng, gt, vt, gb, vb, fg, wg_hbm, wv_hbm, dn_hbm,
    out,
    wg, wv, dn, cur, u, part, rs_send, rs_recv, hid, acc, scale,
    sq_send, sq_recv, tbuf, rbuf, snew,
    wsem, wlate, dsem, rs_ss, rs_rs, ag_ss, ag_rs, sq_ss, sq_rs, t_ss, t_rs, n_ss, n_rs,
):
    n, m, width, length = dims
    layers, dl, ff = wg.shape
    groups, rows, _ = cur.shape
    chunks = part.shape[2]
    cw = ff // 2 // chunks
    rq = rows // m
    me = lax.axis_index("ra")
    mc = lax.axis_index("cb")
    head = SKEW * (n - 1)
    t_term = chunks + head + SKEW_BACK * (n - 1)
    t_own = t_term + SKEW_CB
    t_back = t_own + SKEW_CB
    per_layer = t_back + 1
    lag = per_layer // groups
    f32 = jnp.float32

    def wcopy(d, c, which):
        src, dst = ((wg_hbm, wg), (wv_hbm, wv))[which]
        cols = pl.ds(pl.multiple_of(d * (ff // 2) + c * cw, LANES), cw)
        return pltpu.make_async_copy(src.at[0, :, cols], dst.at[0, :, cols], wsem.at[which, d, c])

    def late(l, which):
        src, dst = ((wg_hbm, wg), (wv_hbm, wv))[which]
        return pltpu.make_async_copy(src.at[l], dst.at[l], wlate.at[which, l])

    def dcopy(l):
        return pltpu.make_async_copy(dn_hbm.at[l], dn.at[l], dsem.at[l])

    for c in range(chunks):
        for d in range(2):
            for which in range(2):
                wcopy(d, c, which).start()

    barrier = pltpu.get_barrier_semaphore()
    for o in range(1, n):
        pl.semaphore_signal(barrier, inc=1, device_id={"ra": lax.rem(me + o, n)}, device_id_type=MESH)
    for o in range(1, m):
        pl.semaphore_signal(barrier, inc=1, device_id={"cb": lax.rem(mc + o, m)}, device_id_type=MESH)
    pl.semaphore_wait(barrier, n + m - 2)

    def remote(src, dst, ss, rs, **to):
        return pltpu.make_async_remote_copy(
            src_ref=src, dst_ref=dst, send_sem=ss, recv_sem=rs, device_id=to, device_id_type=MESH
        )

    def toward(d, back):
        up = (d == 1) != back
        return lax.rem(me + (1 if up else n - 1), n)

    def rs_copy(l, h, d, c):
        return remote(
            rs_send.at[l, h, d, c], rs_recv.at[l, h, d, c], rs_ss.at[l, h, d, c], rs_rs.at[l, h, d, c],
            ra=toward(d, False),
        )

    def ag_copy(l, h, d, c):
        return remote(
            hid.at[l, h, d, c], hid.at[l, h, d, c], ag_ss.at[l, h, d, c], ag_rs.at[l, h, d, c],
            ra=toward(d, True),
        )

    def sq_copy(l, h, o):
        return remote(
            sq_send.at[l, h], sq_recv.at[l, h, o], sq_ss.at[l, h, o], sq_rs.at[l, h, o],
            ra=lax.rem(me + o, n),
        )

    def t_copy(l, h, o):
        to = lax.rem(mc + o, m)
        return remote(
            tbuf.at[l, h, pl.ds(pl.multiple_of(to * rq, rq), rq)], rbuf.at[l, h, o],
            t_ss.at[l, h, o], t_rs.at[l, h, o], cb=to,
        )

    def own(q):
        return pl.ds(pl.multiple_of(q * rq, rq), rq)

    def n_copy(l, h, o):
        mine = own(mc)
        return remote(
            snew.at[l, h, mine], snew.at[l, h, mine], n_ss.at[l, h, o], n_rs.at[l, h, o],
            cb=lax.rem(mc + o, m),
        )

    def n_wait(l, h, o):
        theirs = own(lax.rem(mc + m - o, m))
        remote(
            snew.at[l, h, theirs], snew.at[l, h, theirs], n_ss.at[l, h, o], n_rs.at[l, h, o],
            cb=lax.rem(mc + o, m),
        ).wait_recv()

    def row_of(ref, l, cols=slice(None)):
        block = ref[:, cols].astype(f32)
        row = block[0:1]
        for i in range(1, layers):
            row = jnp.where(l == i, block[i : i + 1], row)
        return row

    def prep(h, l, s):
        cur[h] = s
        values = s.astype(f32)
        u[h] = (values * row_of(ng, l)).astype(jnp.bfloat16)
        total = jnp.sum(values * values, axis=1, keepdims=True)
        square = jnp.broadcast_to(jnp.concatenate([total] * (LANES // rows), axis=0), (LANES, LANES))
        sq_send[l, h] = square.T[0:8]
        for o in range(1, n):
            sq_copy(l, h, o).start()
        acc[h] = jnp.zeros((rows, dl), f32)

    def finish_scale(h, l):
        total = sq_send[l, h]
        for o in range(1, n):
            sq_copy(l, h, o).wait_recv()
            total = total + sq_recv[l, h, o]
        inverse = lax.rsqrt(total / width + EPS)
        scale[h] = jnp.broadcast_to(inverse[0:1], (LANES, LANES)).T[0:rows]

    def down(h, l, d, c):
        at = pl.ds(pl.multiple_of(d * (ff // 2) + c * cw, LANES), cw)
        acc[h] += jnp.dot(hid[l, h, d, c], dn[l, at, :], preferred_element_type=f32)

    def mix(x, taps, bias):
        position = lax.rem(lax.broadcasted_iota(jnp.int32, x.shape, 0), length)
        count = taps.shape[0]
        result = bias + x * taps[count - 1 : count]
        for back in range(1, count):
            moved = jnp.where(position >= back, pltpu.roll(x, back, 0), 0.0)
            result = result + moved * taps[count - 1 - back : count - back]
        return result

    def hidden(h, l, d, c):
        cols = pl.ds(pl.multiple_of(d * (ff // 2) + c * cw, LANES), cw)
        factor = jnp.concatenate([scale[h]] * (cw // LANES), axis=1)
        gate = (part[h, d, c, :, :cw] + rs_recv[l, h, d, c, :, :cw].astype(f32)) * factor
        value = (part[h, d, c, :, cw:] + rs_recv[l, h, d, c, :, cw:].astype(f32)) * factor
        gate = mix(gate, gt[l, :, cols].astype(f32), row_of(gb, l, cols))
        value = mix(value, vt[l, :, cols].astype(f32), row_of(vb, l, cols))
        hid[l, h, d, c] = (jax.nn.gelu(gate) * value).astype(jnp.bfloat16)

    def step(h, l, tau):
        @pl.when(tau < chunks)
        def _():
            for d in range(2):
                if h == 0:

                    @pl.when(l == 0)
                    def _():
                        wcopy(d, tau, 0).wait()
                        wcopy(d, tau, 1).wait()

                    if d == 0:

                        @pl.when((l > 0) & (tau == 0))
                        def _():
                            late(l, 0).wait()
                            late(l, 1).wait()

                cols = pl.ds(pl.multiple_of(d * (ff // 2) + tau * cw, LANES), cw)
                part[h, d, tau, :, :cw] = jnp.dot(u[h], wg[l, :, cols], preferred_element_type=f32)
                part[h, d, tau, :, cw:] = jnp.dot(u[h], wv[l, :, cols], preferred_element_type=f32)

        @pl.when(tau == head)
        def _():
            finish_scale(h, l)
            if h == 0:
                dcopy(l).wait()

        for d in range(2):
            k = me if d == 1 else n - 1 - me
            c = tau - SKEW * k

            @pl.when((c >= 0) & (c < chunks))
            def _():
                @pl.when(k == 0)
                def _():
                    rs_send[l, h, d, c] = part[h, d, c].astype(jnp.bfloat16)
                    rs_copy(l, h, d, c).start()

                @pl.when((k > 0) & (k < n - 1))
                def _():
                    rs_copy(l, h, d, c).wait_recv()
                    rs_send[l, h, d, c] = (part[h, d, c] + rs_recv[l, h, d, c].astype(f32)).astype(jnp.bfloat16)
                    rs_copy(l, h, d, c).start()

                @pl.when(k == n - 1)
                def _():
                    rs_copy(l, h, d, c).wait_recv()
                    hidden(h, l, d, c)
                    ag_copy(l, h, d, c).start()
                    down(h, l, d, c)

        for d in range(2):
            j = n - 1 - me if d == 1 else me
            c = tau - head - SKEW_BACK * j

            @pl.when((j > 0) & (c >= 0) & (c < chunks))
            def _():
                ag_copy(l, h, d, c).wait_recv()

                @pl.when(j < n - 1)
                def _():
                    ag_copy(l, h, d, c).start()

                down(h, l, d, c)

        @pl.when(tau == t_term)
        def _():
            tbuf[l, h] = acc[h].astype(jnp.bfloat16)
            for o in range(1, m):
                t_copy(l, h, o).start()

        @pl.when(tau == t_own)
        def _():
            mine = own(mc)
            total = tbuf[l, h, mine].astype(f32)
            for o in range(1, m):
                t_copy(l, h, o).wait_recv()
                total = total + rbuf[l, h, o].astype(f32)
            snew[l, h, mine] = (0.5 * cur[h, mine].astype(f32) + total).astype(jnp.bfloat16)
            for o in range(1, m):
                n_copy(l, h, o).start()

        @pl.when(tau == t_back)
        def _():
            for o in range(1, m):
                n_wait(l, h, o)
            prep(h, l + 1, snew[l, h])

    for h in range(groups):
        prep(h, 0, s_in[h * rows : (h + 1) * rows])

    def body(t, carry):
        @pl.when(t == chunks - 1)
        def _():
            for l in range(layers):
                dcopy(l).start()
                if l + 1 < layers:
                    late(l + 1, 0).start()
                    late(l + 1, 1).start()

        for h in range(groups):
            at = t - h * lag

            @pl.when((at >= 0) & (at < layers * per_layer))
            def _():
                l = at // per_layer
                step(h, l, at - l * per_layer)

        return carry

    lax.fori_loop(0, layers * per_layer + (groups - 1) * lag, body, 0)

    for h in range(groups):
        finish_scale(h, layers)
        factor = jnp.concatenate([scale[h]] * (dl // LANES), axis=1)
        out[h * rows : (h + 1) * rows] = (
            cur[h].astype(f32) * factor * fg[...].astype(f32)
        ).astype(jnp.bfloat16)

    def drain(i, carry):
        l = i // chunks
        c = i - l * chunks
        for h in range(groups):
            for d in range(2):
                k = me if d == 1 else n - 1 - me

                @pl.when(k < n - 1)
                def _():
                    rs_copy(l, h, d, c).wait_send()

                @pl.when(k > 0)
                def _():
                    ag_copy(l, h, d, c).wait_send()

        return carry

    lax.fori_loop(0, layers * chunks, drain, 0)
    for h in range(groups):
        for l in range(layers):
            for o in range(1, m):
                t_copy(l, h, o).wait_send()
                n_copy(l, h, o).wait_send()
        for l in range(layers + 1):
            for o in range(1, n):
                sq_copy(l, h, o).wait_send()


def body(n, m, width, stream, norm_gain, gate_weight, value_weight, gate_taps, value_taps,
         gate_bias, value_bias, down_weight, final_gain):
    batch, length, dl = stream.shape
    layers, _, ff = gate_weight.shape
    groups = GROUPS if batch % GROUPS == 0 else 1
    rows = batch * length // groups
    chunks = CHUNKS
    cw = ff // 2 // chunks
    bf16, f32 = jnp.bfloat16, jnp.float32
    vmem = pl.BlockSpec(memory_space=pltpu.VMEM)
    hbm = pl.BlockSpec(memory_space=pl.ANY)
    dma = pltpu.SemaphoreType.DMA
    result = pl.pallas_call(
        functools.partial(chain_kernel, (n, m, width, length)),
        out_shape=jax.ShapeDtypeStruct((batch * length, dl), bf16),
        in_specs=[vmem] * 7 + [hbm] * 3,
        out_specs=vmem,
        scratch_shapes=[
            pltpu.VMEM(gate_weight.shape, bf16),
            pltpu.VMEM(value_weight.shape, bf16),
            pltpu.VMEM(down_weight.shape, bf16),
            pltpu.VMEM((groups, rows, dl), bf16),
            pltpu.VMEM((groups, rows, dl), bf16),
            pltpu.VMEM((groups, 2, chunks, rows, 2 * cw), f32),
            pltpu.VMEM((layers, groups, 2, chunks, rows, 2 * cw), bf16),
            pltpu.VMEM((layers, groups, 2, chunks, rows, 2 * cw), bf16),
            pltpu.VMEM((layers, groups, 2, chunks, rows, cw), bf16),
            pltpu.VMEM((groups, rows, dl), f32),
            pltpu.VMEM((groups, rows, LANES), f32),
            pltpu.VMEM((layers + 1, groups, 8, LANES), f32),
            pltpu.VMEM((layers + 1, groups, n, 8, LANES), f32),
            pltpu.VMEM((layers, groups, rows, dl), bf16),
            pltpu.VMEM((layers, groups, m, rows // m, dl), bf16),
            pltpu.VMEM((layers, groups, rows, dl), bf16),
            dma((2, 2, chunks)),
            dma((2, layers)),
            dma((layers,)),
            dma((layers, groups, 2, chunks)),
            dma((layers, groups, 2, chunks)),
            dma((layers, groups, 2, chunks)),
            dma((layers, groups, 2, chunks)),
            dma((layers + 1, groups, n)),
            dma((layers + 1, groups, n)),
            dma((layers, groups, m)),
            dma((layers, groups, m)),
            dma((layers, groups, m)),
            dma((layers, groups, m)),
        ],
        compiler_params=pltpu.CompilerParams(
            collective_id=0, has_side_effects=True, vmem_limit_bytes=66_000_000
        ),
    )(
        stream.reshape(batch * length, dl), norm_gain, gate_taps, value_taps, gate_bias, value_bias,
        final_gain.reshape(1, dl), gate_weight, value_weight, down_weight,
    )
    return result.reshape(batch, length, dl)


def solution(mesh):
    n, m = mesh.shape["ra"], mesh.shape["cb"]

    def run(stream, *rest):
        specs = (
            P("dp", None, "ra"),
            P(None, "ra"),
            P(None, "ra", "cb"),
            P(None, "ra", "cb"),
            P(None, None, "cb"),
            P(None, None, "cb"),
            P(None, "cb"),
            P(None, "cb"),
            P(None, "cb", "ra"),
            P("ra"),
        )
        return jax.shard_map(
            functools.partial(body, n, m, stream.shape[2]),
            mesh=mesh, in_specs=specs, out_specs=P("dp", None, "ra"), check_vma=False,
        )(stream, *rest)

    return run
```

```python
import functools

import jax
import jax.numpy as jnp
from jax import lax
from jax.experimental import pallas as pl
from jax.experimental.pallas import tpu as pltpu
from jax.sharding import PartitionSpec as P

EPS = 1e-06
MESH = pl.DeviceIdType.MESH
LANES = 128
GROUPS = 2
CHUNKS = 6
SKEW = 2
SKEW_BACK = 2
LAG = 6
SKEW_CB = 2


def chain_kernel(
    dims,
    s_in, ng, gt, vt, gb, vb, fg, wg_hbm, wv_hbm, dn_hbm,
    out,
    wg, wv, dn, cur, u, part, rs_send, rs_recv, hid, acc, scale,
    sq_send, sq_recv, tbuf, rbuf, snew,
    wsem, wlate, dsem, rs_ss, rs_rs, ag_ss, ag_rs, sq_ss, sq_rs, t_ss, t_rs, n_ss, n_rs,
):
    n, m, width, length = dims
    layers, dl, ff = wg.shape
    groups, rows, _ = cur.shape
    chunks = part.shape[2]
    cw = ff // 2 // chunks
    rq = rows // m
    me = lax.axis_index("ra")
    mc = lax.axis_index("cb")
    head = SKEW * (n - 1)
    t_term = chunks + head + SKEW_BACK * (n - 1)
    t_own = t_term + SKEW_CB
    t_back = t_own + SKEW_CB
    per_layer = t_back + 1
    lag = LAG
    f32 = jnp.float32

    def wcopy(d, c, which):
        src, dst = ((wg_hbm, wg), (wv_hbm, wv))[which]
        cols = pl.ds(pl.multiple_of(d * (ff // 2) + c * cw, LANES), cw)
        return pltpu.make_async_copy(src.at[0, :, cols], dst.at[0, :, cols], wsem.at[which, d, c])

    def late(l, which):
        src, dst = ((wg_hbm, wg), (wv_hbm, wv))[which]
        return pltpu.make_async_copy(src.at[l], dst.at[l], wlate.at[which, l])

    def dcopy(l):
        return pltpu.make_async_copy(dn_hbm.at[l], dn.at[l], dsem.at[l])

    for c in range(chunks):
        for d in range(2):
            for which in range(2):
                wcopy(d, c, which).start()

    barrier = pltpu.get_barrier_semaphore()
    for o in range(1, n):
        pl.semaphore_signal(barrier, inc=1, device_id={"ra": lax.rem(me + o, n)}, device_id_type=MESH)
    for o in range(1, m):
        pl.semaphore_signal(barrier, inc=1, device_id={"cb": lax.rem(mc + o, m)}, device_id_type=MESH)
    pl.semaphore_wait(barrier, n + m - 2)

    def remote(src, dst, ss, rs, **to):
        return pltpu.make_async_remote_copy(
            src_ref=src, dst_ref=dst, send_sem=ss, recv_sem=rs, device_id=to, device_id_type=MESH
        )

    def toward(d, back):
        up = (d == 1) != back
        return lax.rem(me + (1 if up else n - 1), n)

    def rs_copy(l, h, d, c):
        return remote(
            rs_send.at[l, h, d, c], rs_recv.at[l, h, d, c], rs_ss.at[l, h, d, c], rs_rs.at[l, h, d, c],
            ra=toward(d, False),
        )

    def ag_copy(l, h, d, c):
        return remote(
            hid.at[l, h, d, c], hid.at[l, h, d, c], ag_ss.at[l, h, d, c], ag_rs.at[l, h, d, c],
            ra=toward(d, True),
        )

    def sq_copy(l, h, o):
        return remote(
            sq_send.at[l, h], sq_recv.at[l, h, o], sq_ss.at[l, h, o], sq_rs.at[l, h, o],
            ra=lax.rem(me + o, n),
        )

    def t_copy(l, h, o):
        to = lax.rem(mc + o, m)
        return remote(
            tbuf.at[l, h, pl.ds(pl.multiple_of(to * rq, rq), rq)], rbuf.at[l, h, o],
            t_ss.at[l, h, o], t_rs.at[l, h, o], cb=to,
        )

    def own(q):
        return pl.ds(pl.multiple_of(q * rq, rq), rq)

    def n_copy(l, h, o):
        mine = own(mc)
        return remote(
            snew.at[l, h, mine], snew.at[l, h, mine], n_ss.at[l, h, o], n_rs.at[l, h, o],
            cb=lax.rem(mc + o, m),
        )

    def n_wait(l, h, o):
        theirs = own(lax.rem(mc + m - o, m))
        remote(
            snew.at[l, h, theirs], snew.at[l, h, theirs], n_ss.at[l, h, o], n_rs.at[l, h, o],
            cb=lax.rem(mc + o, m),
        ).wait_recv()

    def row_of(ref, l, *at):
        block = ref[at].astype(f32)
        row = block[0:1]
        for i in range(1, layers):
            row = jnp.where(l == i, block[i : i + 1], row)
        return row

    def prep(h, l, s):
        cur[h] = s
        values = s.astype(f32)
        u[h] = (values * row_of(ng, l, slice(None), slice(None))).astype(jnp.bfloat16)
        total = jnp.sum(values * values, axis=1, keepdims=True)
        square = jnp.broadcast_to(jnp.concatenate([total] * (LANES // rows), axis=0), (LANES, LANES))
        sq_send[l, h] = square.T[0:8]
        for o in range(1, n):
            sq_copy(l, h, o).start()
        acc[h] = jnp.zeros((rows, dl), f32)

    def finish_scale(h, l):
        total = sq_send[l, h]
        for o in range(1, n):
            sq_copy(l, h, o).wait_recv()
            total = total + sq_recv[l, h, o]
        inverse = lax.rsqrt(total / width + EPS)
        scale[h] = jnp.broadcast_to(inverse[0:1], (LANES, LANES)).T[0:rows]

    def down(h, l, d, c):
        at = pl.ds(pl.multiple_of(d * (ff // 2) + c * cw, LANES), cw)
        acc[h] += jnp.dot(hid[l, h, d, c], dn[l, at, :], preferred_element_type=f32)

    def mix(x, taps, bias):
        position = lax.rem(lax.broadcasted_iota(jnp.int32, x.shape, 0), length)
        count = len(taps)
        result = bias + x * taps[count - 1]
        for back in range(1, count):
            moved = jnp.where(position >= back, pltpu.roll(x, back, 0), 0.0)
            result = result + moved * taps[count - 1 - back]
        return result

    def hidden(h, l, d, c):
        cols = pl.ds(pl.multiple_of(d * (ff // 2) + c * cw, LANES), cw)
        factor = jnp.concatenate([scale[h]] * (cw // LANES), axis=1)
        gate = (part[h, d, c, :, :cw] + rs_recv[l, h, d, c, :, :cw].astype(f32)) * factor
        value = (part[h, d, c, :, cw:] + rs_recv[l, h, d, c, :, cw:].astype(f32)) * factor
        gate = mix(gate, [row_of(gt, l, i, slice(None), cols) for i in range(gt.shape[0])], row_of(gb, l, slice(None), cols))
        value = mix(value, [row_of(vt, l, i, slice(None), cols) for i in range(vt.shape[0])], row_of(vb, l, slice(None), cols))
        hid[l, h, d, c] = (jax.nn.gelu(gate) * value).astype(jnp.bfloat16)

    def step(h, l, tau):
        @pl.when(tau < chunks)
        def _():
            for d in range(2):
                if h == 0:

                    @pl.when(l == 0)
                    def _():
                        wcopy(d, tau, 0).wait()
                        wcopy(d, tau, 1).wait()

                    if d == 0:

                        @pl.when((l > 0) & (tau == 0))
                        def _():
                            late(l, 0).wait()
                            late(l, 1).wait()

                cols = pl.ds(pl.multiple_of(d * (ff // 2) + tau * cw, LANES), cw)
                part[h, d, tau, :, :cw] = jnp.dot(u[h], wg[l, :, cols], preferred_element_type=f32)
                part[h, d, tau, :, cw:] = jnp.dot(u[h], wv[l, :, cols], preferred_element_type=f32)

        @pl.when(tau == head)
        def _():
            finish_scale(h, l)
            if h == 0:
                dcopy(l).wait()

        for d in range(2):
            k = me if d == 1 else n - 1 - me
            c = tau - SKEW * k

            @pl.when((c >= 0) & (c < chunks))
            def _():
                @pl.when(k == 0)
                def _():
                    rs_send[l, h, d, c] = part[h, d, c].astype(jnp.bfloat16)
                    rs_copy(l, h, d, c).start()

                @pl.when((k > 0) & (k < n - 1))
                def _():
                    rs_copy(l, h, d, c).wait_recv()
                    rs_send[l, h, d, c] = (part[h, d, c] + rs_recv[l, h, d, c].astype(f32)).astype(jnp.bfloat16)
                    rs_copy(l, h, d, c).start()

                @pl.when(k == n - 1)
                def _():
                    rs_copy(l, h, d, c).wait_recv()
                    hidden(h, l, d, c)
                    ag_copy(l, h, d, c).start()
                    down(h, l, d, c)

        for d in range(2):
            j = n - 1 - me if d == 1 else me
            c = tau - head - SKEW_BACK * j

            @pl.when((j > 0) & (c >= 0) & (c < chunks))
            def _():
                ag_copy(l, h, d, c).wait_recv()

                @pl.when(j < n - 1)
                def _():
                    ag_copy(l, h, d, c).start()

                down(h, l, d, c)

        @pl.when(tau == t_term)
        def _():
            tbuf[l, h] = acc[h].astype(jnp.bfloat16)
            for o in range(1, m):
                t_copy(l, h, o).start()

        @pl.when(tau == t_own)
        def _():
            mine = own(mc)
            total = tbuf[l, h, mine].astype(f32)
            for o in range(1, m):
                t_copy(l, h, o).wait_recv()
                total = total + rbuf[l, h, o].astype(f32)
            snew[l, h, mine] = (0.5 * cur[h, mine].astype(f32) + total).astype(jnp.bfloat16)
            for o in range(1, m):
                n_copy(l, h, o).start()

        @pl.when(tau == t_back)
        def _():
            for o in range(1, m):
                n_wait(l, h, o)
            prep(h, l + 1, snew[l, h])

    for h in range(groups):
        prep(h, 0, s_in[h * rows : (h + 1) * rows])

    def body(t, carry):
        @pl.when(t == min(chunks - 1, head))
        def _():
            for l in range(layers):
                dcopy(l).start()
                if l + 1 < layers:
                    late(l + 1, 0).start()
                    late(l + 1, 1).start()

        for h in range(groups):
            at = t - h * lag

            @pl.when((at >= 0) & (at < layers * per_layer))
            def _():
                l = at // per_layer
                step(h, l, at - l * per_layer)

        return carry

    lax.fori_loop(0, layers * per_layer + (groups - 1) * lag, body, 0)

    for h in range(groups):
        finish_scale(h, layers)
        factor = jnp.concatenate([scale[h]] * (dl // LANES), axis=1)
        out[h * rows : (h + 1) * rows] = (
            cur[h].astype(f32) * factor * fg[...].astype(f32).reshape(1, dl)
        ).astype(jnp.bfloat16)

    def drain(i, carry):
        l = i // chunks
        c = i - l * chunks
        for h in range(groups):
            for d in range(2):
                k = me if d == 1 else n - 1 - me

                @pl.when(k < n - 1)
                def _():
                    rs_copy(l, h, d, c).wait_send()

                @pl.when(k > 0)
                def _():
                    ag_copy(l, h, d, c).wait_send()

        return carry

    lax.fori_loop(0, layers * chunks, drain, 0)
    for h in range(groups):
        for l in range(layers):
            for o in range(1, m):
                t_copy(l, h, o).wait_send()
                n_copy(l, h, o).wait_send()
        for l in range(layers + 1):
            for o in range(1, n):
                sq_copy(l, h, o).wait_send()


def body(n, m, width, stream, norm_gain, gate_weight, value_weight, gate_taps, value_taps,
         gate_bias, value_bias, down_weight, final_gain):
    batch, length, dl = stream.shape
    layers, _, ff = gate_weight.shape
    groups = GROUPS if batch % GROUPS == 0 else 1
    rows = batch * length // groups
    chunks = CHUNKS
    cw = ff // 2 // chunks
    bf16, f32 = jnp.bfloat16, jnp.float32
    vmem = pl.BlockSpec(memory_space=pltpu.VMEM)
    hbm = pl.BlockSpec(memory_space=pl.ANY)
    dma = pltpu.SemaphoreType.DMA
    result = pl.pallas_call(
        functools.partial(chain_kernel, (n, m, width, length)),
        out_shape=jax.ShapeDtypeStruct((batch * length, dl), bf16),
        in_specs=[vmem] * 7 + [hbm] * 3,
        out_specs=vmem,
        scratch_shapes=[
            pltpu.VMEM(gate_weight.shape, bf16),
            pltpu.VMEM(value_weight.shape, bf16),
            pltpu.VMEM(down_weight.shape, bf16),
            pltpu.VMEM((groups, rows, dl), bf16),
            pltpu.VMEM((groups, rows, dl), bf16),
            pltpu.VMEM((groups, 2, chunks, rows, 2 * cw), f32),
            pltpu.VMEM((layers, groups, 2, chunks, rows, 2 * cw), bf16),
            pltpu.VMEM((layers, groups, 2, chunks, rows, 2 * cw), bf16),
            pltpu.VMEM((layers, groups, 2, chunks, rows, cw), bf16),
            pltpu.VMEM((groups, rows, dl), f32),
            pltpu.VMEM((groups, rows, LANES), f32),
            pltpu.VMEM((layers + 1, groups, 8, LANES), f32),
            pltpu.VMEM((layers + 1, groups, n, 8, LANES), f32),
            pltpu.VMEM((layers, groups, rows, dl), bf16),
            pltpu.VMEM((layers, groups, m, rows // m, dl), bf16),
            pltpu.VMEM((layers, groups, rows, dl), bf16),
            dma((2, 2, chunks)),
            dma((2, layers)),
            dma((layers,)),
            dma((layers, groups, 2, chunks)),
            dma((layers, groups, 2, chunks)),
            dma((layers, groups, 2, chunks)),
            dma((layers, groups, 2, chunks)),
            dma((layers + 1, groups, n)),
            dma((layers + 1, groups, n)),
            dma((layers, groups, m)),
            dma((layers, groups, m)),
            dma((layers, groups, m)),
            dma((layers, groups, m)),
        ],
        compiler_params=pltpu.CompilerParams(
            collective_id=0, has_side_effects=True, vmem_limit_bytes=66_000_000
        ),
    )(
        stream.reshape(batch * length, dl), norm_gain, gate_taps.swapaxes(0, 1), value_taps.swapaxes(0, 1), gate_bias, value_bias,
        final_gain, gate_weight, value_weight, down_weight,
    )
    return result.reshape(batch, length, dl)


def solution(mesh):
    n, m = mesh.shape["ra"], mesh.shape["cb"]

    def run(stream, *rest):
        specs = (
            P("dp", None, "ra"),
            P(None, "ra"),
            P(None, "ra", "cb"),
            P(None, "ra", "cb"),
            P(None, None, "cb"),
            P(None, None, "cb"),
            P(None, "cb"),
            P(None, "cb"),
            P(None, "cb", "ra"),
            P("ra"),
        )
        return jax.shard_map(
            functools.partial(body, n, m, stream.shape[2]),
            mesh=mesh, in_specs=specs, out_specs=P("dp", None, "ra"), check_vma=False,
        )(stream, *rest)

    return run
```
